32 devices in a mesh: ep: 8 (over z, core), tp: 4 (over y, x).
Axes of the slice: x: 2, y: 2, z: 4, core: 2. Of those that a mesh axis runs over, the one named last changes fastest.
Arguments:
- tokens: bfloat16 [2048, 2048], P('ep', 'tp'), may hold values from -800 to 800
- norm_gain: bfloat16 [2048], P('tp'), may hold values from 0.099609375 to 1.8984375
- w_gate: bfloat16 [8, 2048, 6144], P('ep', None, 'tp'), may hold values from -0.125 to 0.125
- w_up: bfloat16 [8, 2048, 6144], P('ep', None, 'tp'), may hold values from -0.125 to 0.125
- w_down: bfloat16 [8, 6144, 2048], P('ep', 'tp'), may hold values from -1.2757759 to 1.2757759
- routes: int32 [2048, 2], P('ep'), may hold values from 0 to 7, all different within a row; in each aligned block of 256 rows (0 to 255, 256 to 511, ...) at most 128 rows name the same one
- route_weights: float32 [2048, 2], P('ep'), may hold values from 0.1 to 1
- final_gain: bfloat16 [2048], P('tp'), may hold values from 0.099609375 to 1.8984375
Outputs:
- mixed_out: bfloat16 [2048, 2048], P('ep', 'tp')
The draws below stay inside these ranges and needn't reach their ends.
Inputs may be any that keep to these rules, and one draw needn't show every extreme that they name: `routes`: A token's 2 experts differ. Among the tokens of one index of ep (aligned blocks of 256 rows), no expert is named by more than 128 tokens, a bound that some block reaches.
All inputs are finite; a program needn't handle non-finite values.
Results may differ from the reference program's by a relative error of at most 0.017.
Values may be sent and summed in bfloat16 or wider, within the bound.
A program may use at most 64 MiB of HBM per device.

```python
import math
import jax
import jax.numpy as jnp
import numpy as np
from jax import lax

D = 2048
FF = 6144
TOPK = 2
TOK_DEV = 256
EXPERTS = 8
CAP = 128
TOKENS = 2048
N_EP = 8
N_TP = 4


def draw_tokens(key, part):
    first, second = jax.random.split(jax.random.fold_in(key, 11))
    scales = 10.0 ** jax.random.uniform(first, (TOKENS, 1), jnp.float32)
    columns = 10.0 ** (jnp.arange(D, dtype=jnp.float32) / (D - 1))
    base = jnp.clip(jax.random.normal(second, (TOKENS, D), jnp.float32), -4.0, 4.0)
    return (base * scales * columns[None, :]).astype(jnp.bfloat16)


def draw_w_down(key, part):
    first = jax.random.fold_in(jax.random.fold_in(key, 23), 0)
    columns = jnp.arange(D, dtype=jnp.float32) / (D - 1)
    scales = 10.0 ** columns
    base = jnp.clip(jax.random.normal(first, (EXPERTS, FF, D), jnp.float32), -4.0, 4.0)
    return (base * scales[None, None, :] * FF ** (-0.5)).astype(jnp.bfloat16)


def steps_of(stream_key, dims, pieces, smallest, largest):
    loudness, own = 1.0, jax.random.fold_in(stream_key, 6)
    for axis_at, blocks in pieces:
        draws = jnp.exp(jax.random.uniform(jax.random.fold_in(own, axis_at), (blocks,), jnp.float32, smallest / len(pieces), largest / len(pieces)))
        loudness = loudness * jnp.repeat(draws, dims[axis_at] // blocks).reshape([-1 if axis == axis_at else 1 for axis in range(len(dims))])
    return loudness


def deal_out(key, own, number, rows, count, top, limit, skew):
    sequence = jax.random.permutation(key, count)
    crowded, common = load_shares(count, rows * top, limit, skew, True), load_shares(count, rows * top, limit, skew, False)
    places = jnp.arange(count)

    def named(sizes, rotation):
        used = int((sizes > 0).sum())
        fixed = max(1, used // 4)
        shifted = fixed + (places - fixed + rotation * (used - fixed)) % max(1, count - fixed)
        return jnp.zeros((count,), jnp.int32).at[sequence[jnp.where(places < fixed, places, shifted)]].set(jnp.asarray(sizes, jnp.int32))

    sizes = jnp.where(number % 4 == 0, named(crowded, number // 4), named(common, number - number // 4 - 1))
    mixed = jax.random.permutation(jax.random.fold_in(own, 3), count)
    donor, sink = mixed[0:count // 2 * 2:2], mixed[1:count // 2 * 2:2]
    slack = jnp.minimum(sizes[donor] - 1, limit - sizes[sink]) // 2
    slack = jnp.where((donor == sequence[0]) | (sink == sequence[0]) | (sizes[sink] == 0), 0, jnp.maximum(slack, 0))
    shifted = jax.random.randint(jax.random.fold_in(own, 4), (count // 2,), 0, 1 << 20) % (slack + 1)
    sizes = sizes.at[donor].add(-shifted).at[sink].add(shifted)
    labels = jnp.searchsorted(jnp.cumsum(sizes), jnp.arange(rows * top), side="right").astype(jnp.int32)
    grid = labels.reshape(top, rows).T
    grid = grid[jax.random.permutation(jax.random.fold_in(own, 1), rows)]
    rotation = jax.random.randint(jax.random.fold_in(own, 2), (rows, 1), 0, top)
    return jnp.take_along_axis(grid, (jnp.arange(top)[None, :] + rotation) % top, axis=1)


def load_shares(count, total, limit, slope, full):
    portions = [(1 << 20) // math.isqrt(rank ** slope) + 1 for rank in range(1, count + 1)]
    largest = limit if full else min(limit, max(-(-total // count), total * portions[0] // sum(portions)))
    least = 1 if total - largest >= count - 1 else 0
    given, spare = [largest] + [least] * (count - 1), total - largest - least * (count - 1)
    while spare > 0:
        free = [i for i in range(1, count) if given[i] < largest] or [i for i in range(1, count) if given[i] < limit]
        mass, budget = sum([portions[i] for i in free]), spare
        for i in free:
            extra = min(limit - given[i], max(1, budget * portions[i] // mass), spare)
            given[i] = given[i] + extra
            spare = spare - extra
    return np.array(given)


def scatter_about(key, dims, spread, limit, pieces=(), kind=jnp.bfloat16):
    drawn = spread * jax.random.normal(key, dims, jnp.float32)
    if pieces:
        drawn = drawn * steps_of(key, dims, pieces, -0.22, 0.18)
    return jnp.clip(drawn, -limit, limit).astype(kind)


def setup_inputs(seed: int = 0) -> dict:
    streams_of = jax.random.split(jax.random.key(seed), 9)
    tokens = draw_tokens(jax.random.fold_in(streams_of[8], 71), 0)
    norm_gain = jnp.clip(1.0 + 0.18 * jax.random.normal(streams_of[1], (D,), jnp.float32), 0.099609375, 1.8984375).astype(jnp.bfloat16)
    w_gate = scatter_about(streams_of[2], (EXPERTS, D, FF), D ** -0.5, 0.125, ((0, 8), (2, 4)))
    w_up = scatter_about(streams_of[3], (EXPERTS, D, FF), D ** -0.5, 0.125, ((0, 8), (2, 4)))
    w_down = draw_w_down(jax.random.fold_in(streams_of[8], 71), 0)
    routes_keys = jax.random.split(jax.random.fold_in(streams_of[5], 1), TOKENS // TOK_DEV)
    routes_turns = jax.random.permutation(jax.random.fold_in(streams_of[5], 3), TOKENS // TOK_DEV)
    routes = jax.vmap(lambda own, number: deal_out(jax.random.fold_in(streams_of[5], 2), own, number, TOK_DEV, EXPERTS, TOPK, CAP, 2))(routes_keys, routes_turns).reshape((TOKENS, TOPK))
    route_weights = jnp.clip(0.1 + 0.9 * jax.random.uniform(streams_of[6], (TOKENS, TOPK), jnp.float32) ** steps_of(streams_of[6], (TOKENS, TOPK), ((0, 8),), -0.2, 0.2), 0.1, 1.0)
    final_gain = jnp.clip(1.0 + 0.18 * jax.random.normal(streams_of[7], (D,), jnp.float32), 0.099609375, 1.8984375).astype(jnp.bfloat16)
    return {"tokens": tokens, "norm_gain": norm_gain, "w_gate": w_gate, "w_up": w_up, "w_down": w_down, "routes": routes, "route_weights": route_weights, "final_gain": final_gain}


EPS = 1e-06

def reference(tokens, norm_gain, w_gate, w_up, w_down, routes, route_weights, final_gain):
    wide = tokens.astype(jnp.float32)
    scale = lax.rsqrt(lax.optimization_barrier(jnp.mean(wide * wide, axis=1, keepdims=True)) + EPS)
    normed = (wide * scale * norm_gain.astype(jnp.float32)[None, :]).astype(jnp.bfloat16)
    groups = routes.reshape(N_EP, TOK_DEV * TOPK)
    onehot = (groups[:, :, None] == jnp.arange(EXPERTS, dtype=jnp.int32)[None, None, :]).astype(jnp.int32)
    before = jnp.cumsum(onehot, axis=1) - onehot
    slot = lax.optimization_barrier(jnp.sum(before * onehot, axis=2)).astype(jnp.int32)
    source = jnp.broadcast_to(jnp.arange(N_EP, dtype=jnp.int32)[:, None], groups.shape)
    token_ids = jnp.repeat(jnp.arange(TOKENS, dtype=jnp.int32), TOPK).reshape(N_EP, TOK_DEV * TOPK)
    buffer = jnp.zeros((EXPERTS, N_EP, CAP, D), jnp.bfloat16)
    buffer = buffer.at[groups, source, slot].set(normed[token_ids])

    def one_expert(args):
        rows, gate_w, up_w, down_w = args
        rows = rows.reshape(N_EP * CAP, D).astype(jnp.float32)
        gate = jnp.dot(rows, gate_w.astype(jnp.float32), preferred_element_type=jnp.float32)
        up = jnp.dot(rows, up_w.astype(jnp.float32), preferred_element_type=jnp.float32)
        hidden = (jax.nn.silu(gate) * up).astype(jnp.bfloat16)
        blocks = hidden.reshape(N_EP * CAP, N_TP, FF // N_TP).astype(jnp.float32)
        down_blocks = down_w.reshape(N_TP, FF // N_TP, D).astype(jnp.float32)
        parts = jnp.einsum('rbf,bfd->brd', blocks, down_blocks).astype(jnp.bfloat16)
        return lax.optimization_barrier(jnp.sum(parts.astype(jnp.float32), axis=0)).astype(jnp.bfloat16)
    results = lax.map(one_expert, (buffer, w_gate, w_up, w_down))
    results = results.reshape(EXPERTS, N_EP, CAP, D)
    picked = results[groups, source, slot].reshape(TOKENS, TOPK, D)
    combined = jnp.einsum('tkd,tk->td', picked.astype(jnp.float32), route_weights)
    final_scale = lax.rsqrt(lax.optimization_barrier(jnp.mean(combined * combined, axis=1, keepdims=True)) + EPS)
    return (combined * final_scale * final_gain.astype(jnp.float32)[None, :]).astype(jnp.bfloat16)
```

```python
import functools

import jax
import jax.numpy as jnp
from jax import lax
from jax.experimental import pallas as pl
from jax.experimental.pallas import tpu as pltpu
from jax.sharding import PartitionSpec as P

EPS = 1e-06
VMEM_LIMIT = 60 * 1024 * 1024
F32, BF16 = jnp.float32, jnp.bfloat16


def slot_targets(routes, experts, capacity):
    flat = routes.reshape(-1)
    onehot = (flat[:, None] == jnp.arange(experts, dtype=jnp.int32)[None, :]).astype(jnp.int32)
    before = jnp.cumsum(onehot, axis=0) - onehot
    slot = jnp.sum(before * onehot, axis=1)
    return flat * capacity + slot


def local(tokens, norm_gain, w_gate, w_up, w_down, routes, route_weights, final_gain):
    experts = lax.axis_size("ep")
    tok_rows = tokens.shape[0]
    share = tokens.shape[1]
    width = share * lax.axis_size("tp")
    topk = routes.shape[1]
    capacity = 2 * tok_rows * topk // experts
    wide = tokens.astype(jnp.float32)
    input_squares = lax.psum(jnp.sum(wide * wide, axis=1), "tp")
    scale = lax.rsqrt(input_squares / width + EPS)
    normed = (wide * scale[:, None] * norm_gain.astype(jnp.float32)[None, :]).astype(jnp.bfloat16)
    target = slot_targets(routes, experts, capacity)
    sources = jnp.repeat(jnp.arange(tok_rows, dtype=jnp.int32), topk)
    gate_w = w_gate[0]
    up_w = w_up[0]
    down_w = w_down[0]
    outbox = jnp.zeros((experts * capacity, share), jnp.bfloat16).at[target].set(normed[sources])
    inbox = lax.all_to_all(outbox, "ep", split_axis=0, concat_axis=0, tiled=True)
    piece = lax.all_gather(inbox, "tp", axis=1, tiled=True)
    gate = jnp.dot(piece, gate_w, preferred_element_type=jnp.float32)
    up = jnp.dot(piece, up_w, preferred_element_type=jnp.float32)
    hidden = (jax.nn.silu(gate) * up).astype(jnp.bfloat16)
    sums = lax.psum_scatter(
        lax.dot_general(
            down_w, hidden, (((0,), (1,)), ((), ())), preferred_element_type=jnp.float32
        ).astype(jnp.bfloat16),
        "tp",
        scatter_dimension=0,
        tiled=True,
    )
    returned = lax.all_to_all(sums, "ep", split_axis=1, concat_axis=1, tiled=True)
    picked = jnp.take(returned, target, axis=1).reshape(returned.shape[0], tok_rows, topk)
    combined = jnp.einsum("dtk,tk->td", picked.astype(jnp.float32), route_weights)
    local_squares = jnp.sum(combined * combined, axis=1)
    total_squares = lax.psum(local_squares, "tp")
    final_scale = lax.rsqrt(total_squares / width + EPS)
    return (combined * final_scale[:, None] * final_gain.astype(jnp.float32)[None, :]).astype(
        jnp.bfloat16
    )


def remote(src, dst, send, recv, device):
    return pltpu.make_async_remote_copy(
        src_ref=src, dst_ref=dst, send_sem=send, recv_sem=recv,
        device_id=device, device_id_type=pl.DeviceIdType.MESH,
    )


def kernel(
    n_ep, tokens, gain, wg_hbm, wu_hbm, wd_hbm, routes, weights, final_gain, out,
    wg, wu, wd, pick, outbox, xbuf, gbuf, normed, hidden, pbuf, r1, s1, r2, fin, ret, stat,
    w_sem, z_send, z_recv, ag_send, ag_recv, g_send, g_recv, r1_send, r1_recv,
    r2_send, r2_recv, ret_send, ret_recv, st_send, st_recv,
):
    rows, share = tokens.shape
    topk = routes.shape[1]
    cap = outbox.shape[1]
    width = 4 * share
    pairs = n_ep // 2
    me, q = lax.axis_index("ep"), lax.axis_index("tp")
    nx, ny, nd = q + 1 - 2 * (q % 2), q + 2 - 4 * (q // 2), 3 - q
    tp_peers = (nx, ny, nd)

    def flip(k):
        total, bit = 0, 1
        while bit < n_ep:
            total = total + bit * ((me // bit + k // bit) % 2)
            bit *= 2
        return total

    loads = [
        pltpu.make_async_copy(src, dst, w_sem.at[i])
        for i, (src, dst) in enumerate(((wg_hbm, wg), (wu_hbm, wu), (wd_hbm, wd)))
    ]
    for load in loads:
        load.start()

    barrier = pltpu.get_barrier_semaphore()
    for k in range(1, n_ep):
        pl.semaphore_signal(barrier, inc=1, device_id={"ep": flip(k)}, device_id_type=pl.DeviceIdType.MESH)
    for peer in tp_peers:
        pl.semaphore_signal(barrier, inc=1, device_id={"tp": peer}, device_id_type=pl.DeviceIdType.MESH)

    lane = lax.broadcasted_iota(jnp.int32, (rows, 128), 1)
    named = [routes[:, k : k + 1] for k in range(topk)]
    hot = sum((lane == named[k]).astype(F32) for k in range(topk)).astype(BF16)
    earlier = (
        lax.broadcasted_iota(jnp.int32, (rows, rows), 1) < lax.broadcasted_iota(jnp.int32, (rows, rows), 0)
    ).astype(F32).astype(BF16)
    before = jnp.dot(earlier, hot, preferred_element_type=F32)
    column = lax.broadcasted_iota(jnp.int32, (rows, n_ep * cap), 1)
    for k in range(topk):
        slot = jnp.sum(jnp.where(lane == named[k], before, 0.0), axis=1, keepdims=True)
        target = named[k] * cap + slot.astype(jnp.int32)
        pick[k] = (column == target).astype(F32).astype(BF16)
    for e in range(n_ep):
        both = sum(pick[k, :, e * cap : (e + 1) * cap].astype(F32) for k in range(topk)).astype(BF16)
        outbox[e] = lax.dot_general(
            both, tokens[...], (((0,), (0,)), ((), ())), preferred_element_type=F32
        ).astype(BF16)
    gbuf[q] = gain[...]
    xbuf[me, q] = outbox[me]
    pl.semaphore_wait(barrier, n_ep - 1 + 3)

    def gain_copy(i):
        return remote(gain, gbuf.at[q], g_send.at[i], g_recv.at[i], {"tp": tp_peers[i]})

    def out_copy(k):
        c = flip(k)
        return remote(outbox.at[c], xbuf.at[me, q], z_send.at[k], z_recv.at[k], {"ep": c})

    def spread(k, i, relay=None):
        c = flip(k)
        if i < 2:
            piece, to = q, (nx, ny)[i]
        else:
            piece, to = (ny, nx) [relay], (nx, ny)[relay]
        return remote(xbuf.at[c, piece], xbuf.at[c, piece], ag_send.at[k, i], ag_recv.at[k, i], {"tp": to})

    def first_sum(k, i, p):
        c = flip(k)
        to = (nx, ny)[p]
        return remote(
            pbuf.at[c, (to, nd)[i]], r1.at[c, i], r1_send.at[k, i], r1_recv.at[k, i], {"tp": to}
        )

    def second_sum(k, p):
        c = flip(k)
        return remote(s1.at[c], r2.at[c], r2_send.at[k], r2_recv.at[k], {"tp": (ny, nx)[p]})

    def back(k):
        c = flip(k)
        return remote(fin.at[c], ret.at[me], ret_send.at[k], ret_recv.at[k], {"ep": c})

    def gather_first(s):
        for p in range(2):
            k = 2 * s + p
            if p == 0:
                @pl.when(s > 0)
                def _():
                    out_copy(k).wait_recv()
            else:
                out_copy(k).wait_recv()
            spread(k, p).start()
            spread(k, 1 - p).start()

    def gather_second(s):
        for p in range(2):
            k = 2 * s + p
            spread(k, p).wait_recv()
            spread(k, 2, 1 - p).start()

    def compute(s):
        for p in range(2):
            k = 2 * s + p
            c = flip(k)
            spread(k, 1 - p).wait_recv()
            spread(k, 2, 1 - p).wait_recv()
            squares = jnp.zeros((cap, 1), F32)
            for j in range(4):
                wide = xbuf[c, j].astype(F32)
                squares = squares + jnp.sum(wide * wide, axis=1, keepdims=True)
            scale = lax.rsqrt(squares / width + EPS)
            for j in range(4):
                normed[p * cap : (p + 1) * cap, j * share : (j + 1) * share] = (
                    xbuf[c, j].astype(F32) * scale * gbuf[j, 0:1, :]
                ).astype(BF16)

        @pl.when(s == 0)
        def _():
            loads[0].wait()
            loads[1].wait()

        tile = 256

        @pl.loop(0, wg.shape[1] // tile)
        def _(t):
            cols = pl.ds(pl.multiple_of(t * tile, tile), tile)
            gate = jnp.dot(normed[...], wg[:, cols], preferred_element_type=F32)
            up = jnp.dot(normed[...], wu[:, cols], preferred_element_type=F32)
            hidden[:, cols] = (gate / (1.0 + jnp.exp(-gate)) * up).astype(BF16)

        @pl.when(s == 0)
        def _():
            loads[2].wait()

        @pl.loop(0, 4)
        def _(j):
            cols = pl.ds(pl.multiple_of(j * share, share), share)
            part = jnp.dot(hidden[...], wd[:, cols], preferred_element_type=F32).astype(BF16)
            for p in range(2):
                pbuf[flip(2 * s + p), j] = part[p * cap : (p + 1) * cap]

        for i in (1, 0):
            for p in range(2):
                first_sum(2 * s + p, i, p).start()

    def reduce_first(s):
        for p in range(2):
            k = 2 * s + p
            c = flip(k)
            first_sum(k, 1, p).wait_recv()
            s1[c] = (pbuf[c, (ny, nx)[p]].astype(F32) + r1[c, 1].astype(F32)).astype(BF16)
            second_sum(k, p).start()

    def reduce_second(s):
        for p in range(2):
            k = 2 * s + p
            c = flip(k)
            first_sum(k, 0, p).wait_recv()
            second_sum(k, p).wait_recv()
            total = (pbuf[c, q].astype(F32) + r1[c, 0].astype(F32) + r2[c].astype(F32)).astype(BF16)
            if p == 0:
                @pl.when(s == 0)
                def _():
                    ret[me] = total

                @pl.when(s > 0)
                def _():
                    fin[c] = total
                    back(k).start()
            else:
                fin[c] = total
                back(k).start()

    for k in range(1, n_ep):
        out_copy(k).start()
    for i in range(3):
        gain_copy(i).start()
    gather_first(0)
    gather_first(1)
    gather_second(0)
    gather_first(2)
    for i in range(3):
        gain_copy(i).wait_recv()

    @pl.loop(0, pairs + 2)
    def _(s):
        @pl.when(s < pairs)
        def _():
            compute(s)

        @pl.when(s + 1 < pairs)
        def _():
            gather_second(s + 1)

        @pl.when(s + 3 < pairs)
        def _():
            gather_first(s + 3)

        @pl.when((s >= 1) & (s < pairs + 1))
        def _():
            reduce_first(s - 1)

        @pl.when(s >= 2)
        def _():
            reduce_second(s - 2)

    for k in range(1, n_ep):
        back(k).wait_recv()
    combined = jnp.zeros((rows, share), F32)
    for k in range(topk):
        rowsof = jnp.dot(
            pick[k], ret[...].reshape(n_ep * cap, share), preferred_element_type=F32
        )
        combined = combined + rowsof * weights[:, k : k + 1]
    squares = jnp.sum(combined * combined, axis=1, keepdims=True)
    same = lax.broadcasted_iota(jnp.int32, (rows, rows), 0) == lax.broadcasted_iota(jnp.int32, (rows, rows), 1)
    line = jnp.sum(jnp.where(same, squares, 0.0), axis=0, keepdims=True)
    stat[0] = jnp.broadcast_to(line, (8, rows))

    def stat_copy(i):
        return remote(stat.at[0], stat.at[1 + i], st_send.at[i], st_recv.at[i], {"tp": tp_peers[i]})

    for i in range(3):
        stat_copy(i).start()
    for i in range(3):
        stat_copy(i).wait_recv()
    total = stat[0, 0:1] + stat[1, 0:1] + stat[2, 0:1] + stat[3, 0:1]
    scale = lax.rsqrt(jnp.sum(jnp.where(same, total, 0.0), axis=1, keepdims=True) / width + EPS)
    out[...] = (combined * scale * final_gain[0:1, :]).astype(BF16)

    for i in range(3):
        gain_copy(i).wait_send()
        stat_copy(i).wait_send()
    out_copy(1).wait_send()
    back(1).wait_send()

    @pl.loop(2, n_ep)
    def _(k):
        out_copy(k).wait_send()
        back(k).wait_send()

    @pl.loop(0, pairs)
    def _(s):
        for p in range(2):
            k = 2 * s + p
            spread(k, 0).wait_send()
            spread(k, 1).wait_send()
            spread(k, 2, 1 - p).wait_send()
            first_sum(k, 0, p).wait_send()
            first_sum(k, 1, p).wait_send()
            second_sum(k, p).wait_send()


def fused(tokens, norm_gain, w_gate, w_up, w_down, routes, route_weights, final_gain):
    n_ep = lax.axis_size("ep")
    rows, share = tokens.shape
    topk = routes.shape[1]
    cap = 2 * rows * topk // n_ep
    depth, units = w_gate.shape[1:]
    dma = pltpu.SemaphoreType.DMA
    vmem = pl.BlockSpec(memory_space=pltpu.VMEM)
    hbm = pl.BlockSpec(memory_space=pl.ANY)
    gain8 = jnp.broadcast_to(norm_gain.astype(F32)[None, :], (8, share))
    last8 = jnp.broadcast_to(final_gain.astype(F32)[None, :], (8, share))
    return pl.pallas_call(
        functools.partial(kernel, n_ep),
        out_shape=jax.ShapeDtypeStruct((rows, share), BF16),
        in_specs=[vmem, vmem, hbm, hbm, hbm, vmem, vmem, vmem],
        out_specs=vmem,
        scratch_shapes=[
            pltpu.VMEM((depth, units), BF16),
            pltpu.VMEM((depth, units), BF16),
            pltpu.VMEM((units, depth), BF16),
            pltpu.VMEM((topk, rows, n_ep * cap), BF16),
            pltpu.VMEM((n_ep, cap, share), BF16),
            pltpu.VMEM((n_ep, 4, cap, share), BF16),
            pltpu.VMEM((4, 8, share), F32),
            pltpu.VMEM((2 * cap, depth), BF16),
            pltpu.VMEM((2 * cap, units), BF16),
            pltpu.VMEM((n_ep, 4, cap, share), BF16),
            pltpu.VMEM((n_ep, 2, cap, share), BF16),
            pltpu.VMEM((n_ep, cap, share), BF16),
            pltpu.VMEM((n_ep, cap, share), BF16),
            pltpu.VMEM((n_ep, cap, share), BF16),
            pltpu.VMEM((n_ep, cap, share), BF16),
            pltpu.VMEM((4, 8, rows), F32),
            dma((3,)), dma((n_ep,)), dma((n_ep,)), dma((n_ep, 3)), dma((n_ep, 3)),
            dma((3,)), dma((3,)), dma((n_ep, 2)), dma((n_ep, 2)),
            dma((n_ep,)), dma((n_ep,)), dma((n_ep,)), dma((n_ep,)), dma((3,)), dma((3,)),
        ],
        compiler_params=pltpu.CompilerParams(
            collective_id=0, has_side_effects=True, vmem_limit_bytes=VMEM_LIMIT
        ),
        name="routed_experts",
    )(tokens, gain8, w_gate[0], w_up[0], w_down[0], routes, route_weights, last8)


def solution(mesh):
    in_specs = (
        P("ep", "tp"),
        P("tp"),
        P("ep", None, "tp"),
        P("ep", None, "tp"),
        P("ep", "tp", None),
        P("ep", None),
        P("ep", None),
        P("tp"),
    )
    out_specs = P("ep", "tp")
    n_ep, n_tp = mesh.shape["ep"], mesh.shape["tp"]
    square = n_tp == 4 and n_ep >= 8 and n_ep & (n_ep - 1) == 0
    body = fused if square else local
    return jax.shard_map(body, mesh=mesh, in_specs=in_specs, out_specs=out_specs, check_vma=False)
```

```python
import functools

import jax
import jax.numpy as jnp
from jax import lax
from jax.experimental import pallas as pl
from jax.experimental.pallas import tpu as pltpu
from jax.sharding import PartitionSpec as P

EPS = 1e-06
VMEM_LIMIT = 60 * 1024 * 1024
F32, BF16 = jnp.float32, jnp.bfloat16


def slot_targets(routes, experts, capacity):
    flat = routes.reshape(-1)
    onehot = (flat[:, None] == jnp.arange(experts, dtype=jnp.int32)[None, :]).astype(jnp.int32)
    before = jnp.cumsum(onehot, axis=0) - onehot
    slot = jnp.sum(before * onehot, axis=1)
    return flat * capacity + slot


def local(tokens, norm_gain, w_gate, w_up, w_down, routes, route_weights, final_gain):
    experts = lax.axis_size("ep")
    tok_rows = tokens.shape[0]
    share = tokens.shape[1]
    width = share * lax.axis_size("tp")
    topk = routes.shape[1]
    capacity = 2 * tok_rows * topk // experts
    wide = tokens.astype(jnp.float32)
    input_squares = lax.psum(jnp.sum(wide * wide, axis=1), "tp")
    scale = lax.rsqrt(input_squares / width + EPS)
    normed = (wide * scale[:, None] * norm_gain.astype(jnp.float32)[None, :]).astype(jnp.bfloat16)
    target = slot_targets(routes, experts, capacity)
    sources = jnp.repeat(jnp.arange(tok_rows, dtype=jnp.int32), topk)
    gate_w = w_gate[0]
    up_w = w_up[0]
    down_w = w_down[0]
    outbox = jnp.zeros((experts * capacity, share), jnp.bfloat16).at[target].set(normed[sources])
    inbox = lax.all_to_all(outbox, "ep", split_axis=0, concat_axis=0, tiled=True)
    piece = lax.all_gather(inbox, "tp", axis=1, tiled=True)
    gate = jnp.dot(piece, gate_w, preferred_element_type=jnp.float32)
    up = jnp.dot(piece, up_w, preferred_element_type=jnp.float32)
    hidden = (jax.nn.silu(gate) * up).astype(jnp.bfloat16)
    sums = lax.psum_scatter(
        lax.dot_general(
            down_w, hidden, (((0,), (1,)), ((), ())), preferred_element_type=jnp.float32
        ).astype(jnp.bfloat16),
        "tp",
        scatter_dimension=0,
        tiled=True,
    )
    returned = lax.all_to_all(sums, "ep", split_axis=1, concat_axis=1, tiled=True)
    picked = jnp.take(returned, target, axis=1).reshape(returned.shape[0], tok_rows, topk)
    combined = jnp.einsum("dtk,tk->td", picked.astype(jnp.float32), route_weights)
    local_squares = jnp.sum(combined * combined, axis=1)
    total_squares = lax.psum(local_squares, "tp")
    final_scale = lax.rsqrt(total_squares / width + EPS)
    return (combined * final_scale[:, None] * final_gain.astype(jnp.float32)[None, :]).astype(
        jnp.bfloat16
    )


def remote(src, dst, send, recv, device):
    return pltpu.make_async_remote_copy(
        src_ref=src, dst_ref=dst, send_sem=send, recv_sem=recv,
        device_id=device, device_id_type=pl.DeviceIdType.MESH,
    )


def kernel(
    n_ep, tokens, gains, wg_hbm, wu_hbm, wd_hbm, routes, weights, last, out,
    wg, wu, wd, pick, outbox, xbuf, gbuf, normed, hidden, pbuf, r1, s1, r2, fin, ret, stat,
    w_sem, z_send, z_recv, ag_send, ag_recv, g_send, g_recv, r1_send, r1_recv,
    r2_send, r2_recv, ret_send, ret_recv, st_send, st_recv,
):
    rows, share = tokens.shape
    topk = routes.shape[0]
    cap = outbox.shape[1]
    width = 4 * share
    pairs = n_ep // 2
    me, q = lax.axis_index("ep"), lax.axis_index("tp")
    nx, ny, nd = q + 1 - 2 * (q % 2), q + 2 - 4 * (q // 2), 3 - q
    tp_peers = (nx, ny, nd)

    def flip(k):
        total, bit = 0, 1
        while bit < n_ep:
            total = total + bit * ((me // bit + k // bit) % 2)
            bit *= 2
        return total

    loads = [
        pltpu.make_async_copy(src, dst, w_sem.at[i])
        for i, (src, dst) in enumerate(((wg_hbm, wg), (wu_hbm, wu), (wd_hbm, wd)))
    ]
    for load in loads:
        load.start()

    barrier = pltpu.get_barrier_semaphore()
    for k in range(1, n_ep):
        pl.semaphore_signal(barrier, inc=1, device_id={"ep": flip(k)}, device_id_type=pl.DeviceIdType.MESH)
    for peer in tp_peers:
        pl.semaphore_signal(barrier, inc=1, device_id={"tp": peer}, device_id_type=pl.DeviceIdType.MESH)

    same = lax.broadcasted_iota(jnp.int32, (rows, rows), 0) == lax.broadcasted_iota(jnp.int32, (rows, rows), 1)

    def upright(line):
        return jnp.sum(jnp.where(same, line, 0.0), axis=1, keepdims=True)

    lane = lax.broadcasted_iota(jnp.int32, (rows, 128), 1)
    named = [upright(routes[k : k + 1, :].astype(F32)).astype(jnp.int32) for k in range(topk)]
    hot = sum((lane == named[k]).astype(F32) for k in range(topk)).astype(BF16)
    earlier = (
        lax.broadcasted_iota(jnp.int32, (rows, rows), 1) < lax.broadcasted_iota(jnp.int32, (rows, rows), 0)
    ).astype(F32).astype(BF16)
    before = jnp.dot(earlier, hot, preferred_element_type=F32)
    column = lax.broadcasted_iota(jnp.int32, (rows, n_ep * cap), 1)
    for k in range(topk):
        slot = jnp.sum(jnp.where(lane == named[k], before, 0.0), axis=1, keepdims=True)
        target = named[k] * cap + slot.astype(jnp.int32)
        pick[k] = (column == target).astype(F32).astype(BF16)
    gbuf[q] = jnp.broadcast_to(gains[0:1, :].astype(F32), (8, share))

    def chosen(k):
        cols = pl.ds(pl.multiple_of(flip(k) * cap, cap), cap)
        both = sum(pick[i, :, cols].astype(F32) for i in range(topk)).astype(BF16)
        return lax.dot_general(
            both, tokens[...], (((0,), (0,)), ((), ())), preferred_element_type=F32
        ).astype(BF16)

    xbuf[me, q] = chosen(0)
    pl.semaphore_wait(barrier, n_ep - 1 + 3)

    def gain_copy(i):
        return remote(gbuf.at[q], gbuf.at[q], g_send.at[i], g_recv.at[i], {"tp": tp_peers[i]})

    def out_copy(k):
        c = flip(k)
        return remote(outbox.at[c], xbuf.at[me, q], z_send.at[k], z_recv.at[k], {"ep": c})

    def spread(k, i, relay=None):
        c = flip(k)
        if i < 2:
            piece, to = q, (nx, ny)[i]
        else:
            piece, to = (ny, nx) [relay], (nx, ny)[relay]
        return remote(xbuf.at[c, piece], xbuf.at[c, piece], ag_send.at[k, i], ag_recv.at[k, i], {"tp": to})

    def first_sum(k, i, p):
        c = flip(k)
        to = (nx, ny)[p]
        return remote(
            pbuf.at[c, (to, nd)[i]], r1.at[c, i], r1_send.at[k, i], r1_recv.at[k, i], {"tp": to}
        )

    def second_sum(k, p):
        c = flip(k)
        return remote(s1.at[c], r2.at[c], r2_send.at[k], r2_recv.at[k], {"tp": (ny, nx)[p]})

    def back(k):
        c = flip(k)
        return remote(fin.at[c], ret.at[me], ret_send.at[k], ret_recv.at[k], {"ep": c})

    def gather_first(s):
        for p in range(2):
            k = 2 * s + p
            out_copy(k).wait_recv()
            spread(k, p).start()
            spread(k, 1 - p).start()

    def gather_second(s):
        for p in range(2):
            k = 2 * s + p
            spread(k, p).wait_recv()
            spread(k, 2, 1 - p).start()

    def gate_up(s):
        for p in range(2):
            k = 2 * s + p
            c = flip(k)
            spread(k, 1 - p).wait_recv()
            spread(k, 2, 1 - p).wait_recv()
            squares = jnp.zeros((cap, 1), F32)
            for j in range(4):
                wide = xbuf[c, j].astype(F32)
                squares = squares + jnp.sum(wide * wide, axis=1, keepdims=True)
            scale = lax.rsqrt(squares / width + EPS)
            for j in range(4):
                normed[p * cap : (p + 1) * cap, j * share : (j + 1) * share] = (
                    xbuf[c, j].astype(F32) * scale * gbuf[j, 0:1, :]
                ).astype(BF16)

        @pl.when(s == 0)
        def _():
            loads[0].wait()
            loads[1].wait()

        tile = 256

        @pl.loop(0, wg.shape[1] // tile)
        def _(t):
            cols = pl.ds(pl.multiple_of(t * tile, tile), tile)
            gate = jnp.dot(normed[...], wg[:, cols], preferred_element_type=F32)
            up = jnp.dot(normed[...], wu[:, cols], preferred_element_type=F32)
            hidden[:, cols] = (gate / (1.0 + jnp.exp(-gate)) * up).astype(BF16)

    def down(s):
        @pl.when(s == 0)
        def _():
            loads[2].wait()

        @pl.loop(0, 4)
        def _(j):
            cols = pl.ds(pl.multiple_of(j * share, share), share)
            part = jnp.dot(hidden[...], wd[:, cols], preferred_element_type=F32).astype(BF16)
            for p in range(2):
                pbuf[flip(2 * s + p), j] = part[p * cap : (p + 1) * cap]

        for i in (1, 0):
            for p in range(2):
                first_sum(2 * s + p, i, p).start()

    def reduce_first(s):
        for p in range(2):
            k = 2 * s + p
            c = flip(k)
            first_sum(k, 1, p).wait_recv()
            s1[c] = (pbuf[c, (ny, nx)[p]].astype(F32) + r1[c, 1].astype(F32)).astype(BF16)
            second_sum(k, p).start()

    def reduce_second(s):
        for p in range(2):
            k = 2 * s + p
            c = flip(k)
            first_sum(k, 0, p).wait_recv()
            second_sum(k, p).wait_recv()
            total = (pbuf[c, q].astype(F32) + r1[c, 0].astype(F32) + r2[c].astype(F32)).astype(BF16)
            if p == 0:
                @pl.when(s == 0)
                def _():
                    ret[me] = total

                @pl.when(s > 0)
                def _():
                    fin[c] = total
                    back(k).start()
            else:
                fin[c] = total
                back(k).start()

    for i in range(3):
        gain_copy(i).start()
    spread(0, 0).start()
    spread(0, 1).start()
    for k in range(1, n_ep):
        outbox[flip(k)] = chosen(k)
        out_copy(k).start()
        if k == 3:
            out_copy(1).wait_recv()
            spread(1, 1).start()
            spread(1, 0).start()
    gather_second(0)
    gather_first(1)
    for i in range(3):
        gain_copy(i).wait_recv()

    @pl.loop(0, pairs + 2)
    def _(s):
        @pl.when(s < pairs)
        def _():
            gate_up(s)

        @pl.when(s + 1 < pairs)
        def _():
            gather_second(s + 1)

        @pl.when(s + 2 < pairs)
        def _():
            gather_first(s + 2)

        @pl.when(s < pairs)
        def _():
            down(s)

        @pl.when((s >= 1) & (s < pairs + 1))
        def _():
            reduce_first(s - 1)

        @pl.when(s >= 2)
        def _():
            reduce_second(s - 2)

    for k in range(1, n_ep):
        back(k).wait_recv()
    combined = jnp.zeros((rows, share), F32)
    for k in range(topk):
        rowsof = jnp.dot(
            pick[k], ret[...].reshape(n_ep * cap, share), preferred_element_type=F32
        )
        combined = combined + rowsof * upright(weights[k : k + 1, :])
    squares = jnp.sum(combined * combined, axis=1, keepdims=True)
    line = jnp.sum(jnp.where(same, squares, 0.0), axis=0, keepdims=True)
    stat[0] = jnp.broadcast_to(line, (8, rows))

    def stat_copy(i):
        return remote(stat.at[0], stat.at[1 + i], st_send.at[i], st_recv.at[i], {"tp": tp_peers[i]})

    for i in range(3):
        stat_copy(i).start()
    for i in range(3):
        stat_copy(i).wait_recv()
    total = stat[0, 0:1] + stat[1, 0:1] + stat[2, 0:1] + stat[3, 0:1]
    scale = lax.rsqrt(upright(total) / width + EPS)
    out[...] = (combined * scale * last[0:1, :].astype(F32)).astype(BF16)

    for i in range(3):
        gain_copy(i).wait_send()
        stat_copy(i).wait_send()
    out_copy(1).wait_send()
    back(1).wait_send()

    @pl.loop(2, n_ep)
    def _(k):
        out_copy(k).wait_send()
        back(k).wait_send()

    @pl.loop(0, pairs)
    def _(s):
        for p in range(2):
            k = 2 * s + p
            spread(k, 0).wait_send()
            spread(k, 1).wait_send()
            spread(k, 2, 1 - p).wait_send()
            first_sum(k, 0, p).wait_send()
            first_sum(k, 1, p).wait_send()
            second_sum(k, p).wait_send()


def fused(tokens, norm_gain, w_gate, w_up, w_down, routes, route_weights, final_gain):
    n_ep = lax.axis_size("ep")
    rows, share = tokens.shape
    topk = routes.shape[1]
    cap = 2 * rows * topk // n_ep
    depth, units = w_gate.shape[1:]
    dma = pltpu.SemaphoreType.DMA
    vmem = pl.BlockSpec(memory_space=pltpu.VMEM)
    hbm = pl.BlockSpec(memory_space=pl.ANY)
    return pl.pallas_call(
        functools.partial(kernel, n_ep),
        out_shape=jax.ShapeDtypeStruct((rows, share), BF16),
        in_specs=[vmem, vmem, hbm, hbm, hbm, vmem, vmem, vmem],
        out_specs=vmem,
        scratch_shapes=[
            pltpu.VMEM((depth, units), BF16),
            pltpu.VMEM((depth, units), BF16),
            pltpu.VMEM((units, depth), BF16),
            pltpu.VMEM((topk, rows, n_ep * cap), BF16),
            pltpu.VMEM((n_ep, cap, share), BF16),
            pltpu.VMEM((n_ep, 4, cap, share), BF16),
            pltpu.VMEM((4, 8, share), F32),
            pltpu.VMEM((2 * cap, depth), BF16),
            pltpu.VMEM((2 * cap, units), BF16),
            pltpu.VMEM((n_ep, 4, cap, share), BF16),
            pltpu.VMEM((n_ep, 2, cap, share), BF16),
            pltpu.VMEM((n_ep, cap, share), BF16),
            pltpu.VMEM((n_ep, cap, share), BF16),
            pltpu.VMEM((n_ep, cap, share), BF16),
            pltpu.VMEM((n_ep, cap, share), BF16),
            pltpu.VMEM((4, 8, rows), F32),
            dma((3,)), dma((n_ep,)), dma((n_ep,)), dma((n_ep, 3)), dma((n_ep, 3)),
            dma((3,)), dma((3,)), dma((n_ep, 2)), dma((n_ep, 2)),
            dma((n_ep,)), dma((n_ep,)), dma((n_ep,)), dma((n_ep,)), dma((3,)), dma((3,)),
        ],
        compiler_params=pltpu.CompilerParams(
            collective_id=0, has_side_effects=True, vmem_limit_bytes=VMEM_LIMIT
        ),
        name="routed_experts",
    )(
        tokens, norm_gain[None, :], w_gate[0], w_up[0], w_down[0], routes.T, route_weights.T,
        final_gain[None, :],
    )


def solution(mesh):
    in_specs = (
        P("ep", "tp"),
        P("tp"),
        P("ep", None, "tp"),
        P("ep", None, "tp"),
        P("ep", "tp", None),
        P("ep", None),
        P("ep", None),
        P("tp"),
    )
    out_specs = P("ep", "tp")
    n_ep, n_tp = mesh.shape["ep"], mesh.shape["tp"]
    square = n_tp == 4 and n_ep >= 8 and n_ep & (n_ep - 1) == 0
    body = fused if square else local
    return jax.shard_map(body, mesh=mesh, in_specs=in_specs, out_specs=out_specs, check_vma=False)
```
